32 devices in a mesh: sp: 4 (over z), fs: 4 (over y, core), tp: 2 (over x).
Axes of the slice: x: 2, y: 2, z: 4, core: 2. Of those that a mesh axis runs over, the one named last changes fastest.
Arguments:
- tokens: bfloat16 [4, 768, 2048], P('fs', 'sp'), may hold values from -6 to 6
- decay_pace: float32 [4, 768], P('fs', 'sp'), may hold values from 0.5 to 2, as said below
- start_state: float32 [4, 16, 64, 64], P('fs', 'tp'), may hold values from -80 to 80
- norm_gain: float32 [2048], replicated, may hold values from 0.1 to 1.9
- conv_value: bfloat16 [2048, 512], P(('sp', 'fs'), 'tp'), may hold values from -0.125 to 0.125
- conv_admit: bfloat16 [2048, 512], P(('sp', 'fs'), 'tp'), may hold values from -0.125 to 0.125
- conv_gate: bfloat16 [2048, 512], P(('sp', 'fs'), 'tp'), may hold values from -0.125 to 0.125
- state_query: bfloat16 [2048, 1024], P(('sp', 'fs'), 'tp'), may hold values from -0.125 to 0.125
- state_key: bfloat16 [2048, 1024], P(('sp', 'fs'), 'tp'), may hold values from -0.125 to 0.125
- state_value: bfloat16 [2048, 1024], P(('sp', 'fs'), 'tp'), may hold values from -0.125 to 0.125
- state_decay: bfloat16 [2048, 1024], P(('sp', 'fs'), 'tp'), may hold values from -0.125 to 0.125
- state_gate: bfloat16 [2048, 1024], P(('sp', 'fs'), 'tp'), may hold values from -0.125 to 0.125
- conv_taps: float32 [31, 512], P(None, 'tp'), may hold values from -4 to 4
- conv_gain: float32 [512], P('tp'), may hold values from 0.1 to 1.9
- point_weight: bfloat16 [512, 512], replicated, may hold values from -0.25 to 0.25
- decay_base: float32 [1024], P('tp'), may hold values from -13 to -3
- correction: float32 [1024], P('tp'), may hold values from 0 to 0.9
- group_gain: float32 [1024], P('tp'), may hold values from 0.1 to 1.9
- output_conv: bfloat16 [512, 2048], P('tp', ('sp', 'fs')), may hold values from -0.25 to 0.25
- output_state: bfloat16 [1024, 2048], P('tp', ('sp', 'fs')), may hold values from -0.1875 to 0.1875
Outputs:
- mixed: bfloat16 [4, 768, 2048], P('fs', ('sp', 'tp'))
The draws below stay inside these ranges and needn't reach their ends.
Inputs may be any that keep to these rules, and one draw needn't show every extreme that they name: `decay_pace`: constant over runs of positions, a quarter of 192 long.
All inputs are finite; a program needn't handle non-finite values.
Results may differ from the reference program's by a relative error of at most 0.017.
Values may be sent and summed in bfloat16 or wider, within the bound.
A program may use at most 64 MiB of HBM per device.

```python
import jax
import jax.numpy as jnp
from jax import lax

D = 2048
CB = 512
C_HEADS = 16
HEAD = 64
KERNEL = 31
TOK_DEV = 192
C = 1024
SEQ = 768
SEQS = 4


def log_uniform(key, shape, lower, upper):
    fraction = jax.random.uniform(key, shape, jnp.float32)
    return jnp.exp(jnp.log(lower) + fraction * (jnp.log(upper) - jnp.log(lower)))


def fast_channels(key):
    picks = jax.random.randint(jax.random.fold_in(key, 11), (C_HEADS,), 0, 10)
    chosen = picks < 5
    return jnp.repeat(chosen, HEAD)


def draw_decay_base(key, part):
    fast = fast_channels(key)
    slow_rate = log_uniform(jax.random.fold_in(key, 3), (C,), 0.15, 0.8) / SEQ
    fast_rate = log_uniform(jax.random.fold_in(key, 4), (C,), 0.012, 0.04)
    return jnp.clip(jnp.log(jnp.where(fast, fast_rate, slow_rate)), -13.0, -3.0)


def draw_correction(key, part):
    fast = fast_channels(key)
    slow_value = jnp.minimum(log_uniform(jax.random.fold_in(key, 5), (C,), 0.1, 0.6) * HEAD / SEQ, 0.9)
    fast_value = jax.random.uniform(jax.random.fold_in(key, 6), (C,), jnp.float32, 0.2, 0.9)
    return jnp.where(fast, fast_value, slow_value)


def draw_decay_pace(key, part):
    stretch = max(TOK_DEV // 4, 1)
    values = log_uniform(key, (SEQS, SEQ // stretch), 0.5, 2.0)
    return jnp.repeat(values, stretch, axis=1)


def draw_conv_taps(key, part):
    group = max(CB // 16, 1)
    factor = log_uniform(jax.random.fold_in(key, 8), (CB // group,), 1.0 / 3.0, 3.0)
    taps = jax.random.normal(jax.random.fold_in(key, 9), (KERNEL, CB), jnp.float32) * KERNEL ** (-0.5)
    return jnp.clip(taps * jnp.repeat(factor, group)[None, :], -4.0, 4.0)


def block_levels(key, shape, split, low, top_value):
    gain, own = 1.0, jax.random.fold_in(key, 6)
    for axis_at, blocks in split:
        heights = jnp.exp(jax.random.uniform(jax.random.fold_in(own, axis_at), (blocks,), jnp.float32, low / len(split), top_value / len(split)))
        gain = gain * jnp.repeat(heights, shape[axis_at] // blocks).reshape([-1 if axis == axis_at else 1 for axis in range(len(shape))])
    return gain


def bell_draw(stream_key, shape, scale, reach, shards=(), held_as=jnp.bfloat16):
    loudness = block_levels(stream_key, shape, shards, -0.22, 0.18) if shards else 1.0
    values = jax.random.normal(stream_key, shape, jnp.float32) * scale * loudness
    return jnp.minimum(jnp.maximum(values, -reach), reach).astype(held_as)


def setup_inputs(seed: int = 0) -> dict:
    seeds = jax.random.split(jax.random.key(seed), 21)
    return {
        "tokens": bell_draw(seeds[0], (SEQS, SEQ, D), 1.0, 6.0, ((0, 4), (1, 4))),
        "decay_pace": draw_decay_pace(jax.random.fold_in(seeds[20], 71), 0),
        "start_state": bell_draw(seeds[2], (SEQS, C_HEADS, HEAD, HEAD), (0.5 * SEQ ** 0.5), 80.0, ((0, 4), (1, 2)), jnp.float32),
        "norm_gain": jnp.clip(1.0 + 0.18 * jax.random.normal(seeds[3], (D,), jnp.float32), 0.1, 1.9),
        "conv_value": bell_draw(seeds[4], (D, CB), D ** -0.5, 0.125, ((0, 16), (1, 2))),
        "conv_admit": bell_draw(seeds[5], (D, CB), D ** -0.5, 0.125, ((0, 16), (1, 2))),
        "conv_gate": bell_draw(seeds[6], (D, CB), D ** -0.5, 0.125, ((0, 16), (1, 2))),
        "state_query": bell_draw(seeds[7], (D, C), D ** -0.5, 0.125, ((0, 16), (1, 2))),
        "state_key": bell_draw(seeds[8], (D, C), D ** -0.5, 0.125, ((0, 16), (1, 2))),
        "state_value": bell_draw(seeds[9], (D, C), D ** -0.5, 0.125, ((0, 16), (1, 2))),
        "state_decay": bell_draw(seeds[10], (D, C), D ** -0.5, 0.125, ((0, 16), (1, 2))),
        "state_gate": bell_draw(seeds[11], (D, C), D ** -0.5, 0.125, ((0, 16), (1, 2))),
        "conv_taps": draw_conv_taps(jax.random.fold_in(seeds[20], 71), 0),
        "conv_gain": jnp.clip(1.0 + 0.18 * jax.random.normal(seeds[13], (CB,), jnp.float32), 0.1, 1.9),
        "point_weight": bell_draw(seeds[14], (CB, CB), CB ** -0.5, 0.25),
        "decay_base": draw_decay_base(jax.random.fold_in(seeds[20], 71), 0),
        "correction": draw_correction(jax.random.fold_in(seeds[20], 71), 0),
        "group_gain": jnp.clip(1.0 + 0.18 * jax.random.normal(seeds[17], (C,), jnp.float32), 0.1, 1.9),
        "output_conv": bell_draw(seeds[18], (CB, D), CB ** -0.5, 0.25, ((0, 2), (1, 16))),
        "output_state": bell_draw(seeds[19], (C, D), C ** -0.5, 0.1875, ((0, 2), (1, 16))),
    }


NORM_FLOOR = 0.1
CHANNEL_FLOOR = 0.1
GROUP_FLOOR = 1.0

def project(normed_rows, weight, shape):
    return jnp.dot(normed_rows, weight, preferred_element_type=jnp.float32).astype(jnp.bfloat16).reshape(shape)

def reference(tokens, decay_pace, start_state, norm_gain, conv_value, conv_admit, conv_gate, state_query, state_key, state_value, state_decay, state_gate, conv_taps, conv_gain, point_weight, decay_base, correction, group_gain, output_conv, output_state):
    seqs, length, width = tokens.shape
    floats = tokens.astype(jnp.float32)
    inverse = lax.rsqrt(lax.optimization_barrier(jnp.mean(floats * floats, axis=-1, keepdims=True)) + NORM_FLOOR)
    normed = (floats * inverse * norm_gain).astype(jnp.bfloat16).reshape(seqs * length, width)
    conv_shape = (seqs, length, CB)
    value = project(normed, conv_value, conv_shape).astype(jnp.float32)
    admit = project(normed, conv_admit, conv_shape).astype(jnp.float32)
    gate_conv = project(normed, conv_gate, conv_shape).astype(jnp.float32)
    rounded = lax.optimization_barrier((value * jax.nn.sigmoid(admit)).astype(jnp.bfloat16))
    conv_input = rounded.astype(jnp.float32)
    padded = jnp.pad(conv_input, ((0, 0), (KERNEL - 1, 0), (0, 0)))
    conv_sum = jnp.zeros(conv_shape, jnp.float32)
    for offset in range(KERNEL):
        conv_sum = conv_sum + conv_taps[offset] * padded[:, offset:offset + length]
    mean = lax.optimization_barrier(jnp.mean(conv_sum, axis=-1, keepdims=True))
    spread = lax.optimization_barrier(jnp.mean(conv_sum * conv_sum, axis=-1, keepdims=True)) - mean * mean
    shaped = jax.nn.silu((conv_sum - mean) * lax.rsqrt(spread + CHANNEL_FLOOR) * conv_gain).astype(jnp.bfloat16)
    pointwise = jnp.dot(shaped.reshape(-1, CB), point_weight, preferred_element_type=jnp.float32).reshape(conv_shape)
    conv_out = (pointwise * jax.nn.silu(gate_conv)).astype(jnp.bfloat16)
    head_shape = (seqs, length, C_HEADS, HEAD)
    query = project(normed, state_query, head_shape).astype(jnp.float32)
    keys = project(normed, state_key, head_shape).astype(jnp.float32)
    values = project(normed, state_value, head_shape).astype(jnp.float32)
    decay_in = project(normed, state_decay, (seqs, length, C)).astype(jnp.float32)
    gate_state = project(normed, state_gate, (seqs, length, C)).astype(jnp.float32)
    log_keep = -jnp.exp(decay_base + jnp.tanh(decay_in)) * decay_pace[:, :, None]
    keep = jnp.exp(log_keep).reshape(head_shape)
    unit = keys * lax.rsqrt(jnp.maximum(lax.optimization_barrier(jnp.sum(keys * keys, axis=-1, keepdims=True)), 1.0))
    remove = -unit
    write = unit * correction.reshape(C_HEADS, HEAD)

    def advance(state, inputs):
        query_now, keep_now, key_now, value_now, remove_now, write_now = inputs
        removed = jnp.einsum('shvk,shk->shv', state, remove_now, precision=lax.Precision.HIGHEST)
        state = state * keep_now[:, :, None, :] + removed[..., None] * write_now[:, :, None, :] + value_now[..., None] * key_now[:, :, None, :]
        return (state, jnp.einsum('shvk,shk->shv', state, query_now, precision=lax.Precision.HIGHEST))
    inputs = tuple((jnp.moveaxis(array, 1, 0) for array in (query, keep, keys, values, remove, write)))
    final_state, outputs = lax.scan(advance, start_state.astype(jnp.float32), inputs)
    outputs = jnp.moveaxis(outputs, 0, 1)
    centered = outputs - lax.optimization_barrier(jnp.mean(outputs, axis=-1, keepdims=True))
    variance = lax.optimization_barrier(jnp.mean(centered * centered, axis=-1, keepdims=True))
    grouped = centered * lax.rsqrt(variance + GROUP_FLOOR) * group_gain.reshape(C_HEADS, HEAD)
    state_out = (grouped.reshape(seqs, length, C) * jax.nn.silu(gate_state)).astype(jnp.bfloat16)
    joined = jnp.concatenate([conv_out, state_out], axis=-1).reshape(seqs * length, CB + C)
    weight = jnp.concatenate([output_conv, output_state], axis=0)
    mixed = jnp.dot(joined, weight, preferred_element_type=jnp.float32).astype(jnp.bfloat16)
    return mixed.reshape(seqs, length, width)
```

```python
import functools

import jax
import jax.numpy as jnp
from jax import lax
from jax.experimental import pallas as pl
from jax.experimental.pallas import tpu as pltpu
from jax.sharding import PartitionSpec as P

NORM_FLOOR = 0.1
CHANNEL_FLOOR = 0.1
GROUP_FLOOR = 1.0


def passed_along(value, axis, steps):
    count = lax.axis_size(axis)
    leading, last = (max(0, -steps), min(count, count - steps))
    return lax.ppermute(value, axis, [(source, source + steps) for source in range(leading, last)])


def entering_2(value, axis, join, neutral):
    place = lax.axis_index(axis)
    gathered = jax.tree.map(
        lambda a, kind: lax.all_gather(a.astype(kind), axis),
        value,
        jax.tree.map(lambda a: jnp.bfloat16 if a.dtype == jnp.float32 else a.dtype, value),
    )
    state = jax.tree.map(lambda a, e: jnp.zeros_like(a) + jnp.asarray(e, a.dtype), value, neutral)

    def one(lap, state):
        return join(
            state,
            jax.tree.map(
                lambda a, own: lax.dynamic_index_in_dim(a, lap, 0, False).astype(own.dtype),
                gathered,
                value,
            ),
        )

    return lax.fori_loop(0, place, one, state)


def apply_map(matrix, right):
    return jnp.einsum("hbti,hbic->hbtc", matrix, right, precision=lax.Precision.HIGHEST)


def pair_terms(left, right, mask):
    return jnp.einsum("hbtc,hbic->hbti", left, right, precision=lax.Precision.HIGHEST) * mask


def compose(earlier, later):
    first = jnp.matmul(earlier[0], later[0], precision=lax.Precision.HIGHEST)
    second = jnp.matmul(earlier[1], later[0], precision=lax.Precision.HIGHEST) + later[1]
    return (first, second)


def block_terms(query, keys, values, unit, write, log_keep):
    size = query.shape[-1]
    span = query.shape[2]
    total_log = jnp.cumsum(log_keep, axis=2)
    before_log = total_log - log_keep
    last_log = total_log[:, :, span - 1 :, :]
    lead_remove = -unit * jnp.exp(before_log)
    lead_query = query * jnp.exp(total_log)
    back_write = write * jnp.exp(-total_log)
    back_key = keys * jnp.exp(-total_log)
    places = jnp.arange(span)
    strict = (places[:, None] > places[None, :]).astype(jnp.float32)
    weak = (places[:, None] >= places[None, :]).astype(jnp.float32)
    remove_write = pair_terms(lead_remove, back_write, strict)
    remove_key = pair_terms(lead_remove, back_key, strict)
    query_write = pair_terms(lead_query, back_write, weak)
    query_key = pair_terms(lead_query, back_key, weak)
    right_side = jnp.concatenate([apply_map(remove_key, values), lead_remove], axis=-1)
    system = jnp.eye(span, dtype=jnp.float32) - remove_write
    solved = jax.scipy.linalg.solve_triangular(system, right_side, lower=True, unit_diagonal=True)
    own_part = solved[..., :size]
    start_part = solved[..., size:]
    local_out = apply_map(query_write, own_part) + apply_map(query_key, values)
    start_map = lead_query + apply_map(query_write, start_part)
    tail_write = write * jnp.exp(last_log - total_log)
    tail_key = keys * jnp.exp(last_log - total_log)
    carry_map = jnp.einsum(
        "hbtk,hbtj->hbkj", start_part, tail_write, precision=lax.Precision.HIGHEST
    ) + jnp.eye(size, dtype=jnp.float32) * jnp.exp(last_log)
    carry_add = jnp.einsum(
        "hbtv,hbtj->hbvj", own_part, tail_write, precision=lax.Precision.HIGHEST
    ) + jnp.einsum("hbtv,hbtj->hbvj", values, tail_key, precision=lax.Precision.HIGHEST)
    return (local_out, start_map, carry_map, carry_add)


def body(
    tokens,
    decay_pace,
    start_state,
    norm_gain,
    conv_value,
    conv_admit,
    conv_gate,
    state_query,
    state_key,
    state_value,
    state_decay,
    state_gate,
    conv_taps,
    conv_gain,
    point_weight,
    decay_base,
    correction,
    group_gain,
    output_conv,
    output_state,
):
    width = tokens.shape[-1]
    rows = tokens.reshape(-1, width)
    length = rows.shape[0]
    floats = rows.astype(jnp.float32)
    inverse = lax.rsqrt(jnp.mean(floats * floats, axis=1, keepdims=True) + NORM_FLOOR)
    normed = (floats * inverse * norm_gain).astype(jnp.bfloat16)
    shards = (
        conv_value,
        conv_admit,
        conv_gate,
        state_query,
        state_key,
        state_value,
        state_decay,
        state_gate,
    )
    stacked = jnp.concatenate(shards, axis=1)
    projected = jnp.dot(
        normed,
        lax.all_gather(stacked, ("sp", "fs"), axis=0, tiled=True),
        preferred_element_type=jnp.float32,
    ).astype(jnp.bfloat16)
    pieces = []
    offset = 0
    for shard in shards:
        pieces.append(projected[:, offset : offset + shard.shape[1]].astype(jnp.float32))
        offset = offset + shard.shape[1]
    value, admit, gate_conv, query, keys, values, decay_in, gate_state = pieces
    channels = value.shape[1]
    kernel = conv_taps.shape[0]
    conv_input = (value * jax.nn.sigmoid(admit)).astype(jnp.bfloat16)
    earlier = passed_along(conv_input[length - (kernel - 1) :], "sp", 1)
    padded = jnp.concatenate([earlier, conv_input], axis=0).astype(jnp.float32)
    conv_sum = jnp.zeros((length, channels), jnp.float32)
    for place in range(kernel):
        conv_sum = conv_sum + conv_taps[place] * padded[place : place + length]
    local_point = lax.dynamic_slice_in_dim(
        point_weight, lax.axis_index("tp") * channels, channels, 1
    )
    whole_sum, whole_gain = (
        lax.all_gather(conv_sum.astype(jnp.bfloat16), "tp", axis=1, tiled=True).astype(
            conv_sum.dtype
        ),
        lax.all_gather(conv_gain.astype(jnp.bfloat16), "tp", axis=0, tiled=True).astype(
            conv_gain.dtype
        ),
    )
    mean = jnp.mean(whole_sum, axis=1, keepdims=True)
    spread = jnp.mean(whole_sum * whole_sum, axis=1, keepdims=True) - mean * mean
    shaped = jax.nn.silu(
        (whole_sum - mean) * lax.rsqrt(spread + CHANNEL_FLOOR) * whole_gain
    ).astype(jnp.bfloat16)
    pointwise = jnp.dot(shaped, local_point, preferred_element_type=jnp.float32)
    conv_out = (pointwise * jax.nn.silu(gate_conv)).astype(jnp.bfloat16)
    size = start_state.shape[-1]
    heads = query.shape[1] // size
    span = min(64, length)
    blocks = length // span
    log_keep = -jnp.exp(decay_base + jnp.tanh(decay_in)) * decay_pace.reshape(-1)[:, None]
    key_heads = keys.reshape(length, heads, size)
    unit = key_heads * lax.rsqrt(
        jnp.maximum(jnp.sum(key_heads * key_heads, axis=-1, keepdims=True), 1.0)
    )
    write = unit * correction.reshape(heads, size)

    def arrange(array):
        return array.reshape(blocks, span, heads, size).transpose(2, 0, 1, 3)

    local_out, start_map, carry_map, carry_add = block_terms(
        arrange(query),
        arrange(keys),
        arrange(values),
        arrange(unit),
        arrange(write),
        arrange(log_keep),
    )
    identity = (
        jnp.broadcast_to(jnp.eye(size, dtype=jnp.float32), (heads, size, size)),
        jnp.zeros((heads, size, size), jnp.float32),
    )

    def along(carried, block_pair):
        return (compose(carried, block_pair), carried)

    device_pair, prefixes = lax.scan(
        along, identity, (jnp.moveaxis(carry_map, 1, 0), jnp.moveaxis(carry_add, 1, 0))
    )
    prior_map, prior_add = entering_2(device_pair, "sp", compose, identity)
    begin = start_state.reshape(heads, size, size)
    entering = jnp.matmul(begin, prior_map, precision=lax.Precision.HIGHEST) + prior_add
    block_starts = (
        jnp.matmul(entering[None], prefixes[0], precision=lax.Precision.HIGHEST) + prefixes[1]
    )
    block_starts = jnp.moveaxis(block_starts, 0, 1)
    outputs = local_out + jnp.einsum(
        "hbtk,hbvk->hbtv", start_map, block_starts, precision=lax.Precision.HIGHEST
    )
    outputs = outputs.transpose(1, 2, 0, 3).reshape(length, heads, size)
    centered = outputs - jnp.mean(outputs, axis=-1, keepdims=True)
    variance = jnp.mean(centered * centered, axis=-1, keepdims=True)
    grouped = centered * lax.rsqrt(variance + GROUP_FLOOR) * group_gain.reshape(heads, size)
    state_out = (grouped.reshape(length, heads * size) * jax.nn.silu(gate_state)).astype(
        jnp.bfloat16
    )
    local_mix = jnp.concatenate([conv_out, state_out], axis=1)
    moved = lax.all_to_all(local_mix, "tp", split_axis=0, concat_axis=1, tiled=True)
    conv_rows, state_rows = (
        lax.all_gather(output_conv, "tp", axis=0, tiled=True),
        lax.all_gather(output_state, "tp", axis=0, tiled=True),
    )
    groups = lax.axis_size("tp")
    joined = jnp.concatenate(
        [conv_rows.reshape(groups, channels, -1), state_rows.reshape(groups, heads * size, -1)],
        axis=1,
    )
    joined = joined.reshape(groups * (channels + heads * size), -1)
    mixed = jnp.dot(
        moved,
        lax.all_gather(joined, ("sp", "fs"), axis=1, tiled=True),
        preferred_element_type=jnp.float32,
    )
    return mixed.astype(jnp.bfloat16).reshape(1, -1, width)


def halves(array):
    high = array.astype(jnp.bfloat16)
    low = (array - high.astype(jnp.float32)).astype(jnp.bfloat16)
    return (high, low)


def product(left, right, dims=((1,), (0,))):
    def one(a, b):
        return lax.dot_general(a, b, (dims, ((), ())), preferred_element_type=jnp.float32)

    return one(left[0], right[0]) + (one(left[0], right[1]) + one(left[1], right[0]))


def mixer_kernel(
    size,
    span,
    group,
    proj_ref,
    pace_ref,
    base_ref,
    correction_ref,
    gain_ref,
    taps_ref,
    begin_ref,
    out_ref,
    local_ref,
    map_ref,
    carry_ref,
    add_ref,
    conv_ref,
):
    length = proj_ref.shape[0]
    heads = begin_ref.shape[0]
    wide = heads * size
    blocks = length // span
    kernel, channels = taps_ref.shape
    f32 = jnp.float32
    row = lax.broadcasted_iota(jnp.int32, (span, span), 0)
    col = lax.broadcasted_iota(jnp.int32, (span, span), 1)
    strict = (row > col).astype(f32)
    weak = (row >= col).astype(f32)
    masks = jnp.concatenate(
        [jnp.concatenate([strict, strict], axis=1), jnp.concatenate([weak, weak], axis=1)], axis=0
    )
    eye = (row == col).astype(f32)
    square = (
        lax.broadcasted_iota(jnp.int32, (size, size), 0)
        == lax.broadcasted_iota(jnp.int32, (size, size), 1)
    ).astype(f32)
    least = min(8, span)
    same = (row // least == col // least).astype(f32)
    merges = []
    width = least
    while width < span:
        merges.append(
            ((row // (2 * width) == col // (2 * width)) & (row // width != col // width)).astype(f32)
        )
        width = 2 * width
    weak_bf = weak.astype(jnp.bfloat16)

    def step(turn, _):
        items = []
        for part in range(group):
            block = turn * group + part
            rows = pl.ds(pl.multiple_of(block * span, span), span)
            query = proj_ref[rows, 0:wide].astype(f32)
            keys = proj_ref[rows, wide : 2 * wide].astype(f32)
            values = proj_ref[rows, 2 * wide : 3 * wide].astype(f32)
            decay_in = proj_ref[rows, 3 * wide : 4 * wide].astype(f32)
            log_keep = -jnp.exp(base_ref[...] + jnp.tanh(decay_in)) * pace_ref[rows, :]
            high = log_keep.astype(jnp.bfloat16)
            rest = log_keep - high.astype(f32)
            mid = rest.astype(jnp.bfloat16)
            low = (rest - mid.astype(f32)).astype(jnp.bfloat16)
            total = (
                jnp.dot(weak_bf, high, preferred_element_type=f32)
                + jnp.dot(weak_bf, mid, preferred_element_type=f32)
                + jnp.dot(weak_bf, low, preferred_element_type=f32)
            )
            last = total[span - 1 : span, :]
            lead = jnp.exp(total - log_keep)
            grown = jnp.exp(total)
            back = jnp.exp(-total)
            tail = jnp.exp(last - total)
            ended = jnp.exp(last)
            for head in range(heads):
                at = slice(head * size, (head + 1) * size)
                key = keys[:, at]
                unit = key * lax.rsqrt(
                    jnp.maximum(jnp.sum(key * key, axis=1, keepdims=True), 1.0)
                )
                write = unit * correction_ref[:, at]
                lead_remove = -unit * lead[:, at]
                lead_query = query[:, at] * grown[:, at]
                items.append(
                    dict(
                        at=(block, head),
                        value=values[:, at],
                        lead_remove=lead_remove,
                        lead_query=lead_query,
                        left=jnp.concatenate([lead_remove, lead_query], axis=0),
                        right=jnp.concatenate([write * back[:, at], key * back[:, at]], axis=0),
                        tail_write=write * tail[:, at],
                        tail_key=key * tail[:, at],
                        ended=ended[:, at],
                    )
                )
        for item in items:
            item["pair"] = (
                product(halves(item["left"]), halves(item["right"]), ((1,), (1,))) * masks
            )
        for item in items:
            item["system"] = item["pair"][:span, :span]
            item["power"] = halves(item["system"] * same)
            item["inverse"] = eye + item["system"] * same
        width = 2
        while width < least:
            for item in items:
                item["power"] = halves(product(item["power"], item["power"]))
            for item in items:
                item["inverse"] = item["inverse"] + product(
                    halves(item["inverse"]), item["power"]
                )
            width = 2 * width
        for item in items:
            padded = jnp.concatenate([jnp.zeros_like(item["value"]), item["value"]], axis=0)
            item["mixed"] = product(halves(item["pair"]), halves(padded))
        for merge in merges:
            for item in items:
                item["inside"] = halves(item["inverse"])
                item["next"] = halves(product(halves(item["system"] * merge), item["inside"]))
            for item in items:
                item["inverse"] = item["inverse"] + product(item["inside"], item["next"])
        for item in items:
            right_side = jnp.concatenate([item["mixed"][:span], item["lead_remove"]], axis=1)
            item["solved"] = halves(product(halves(item["inverse"]), halves(right_side)))
        for item in items:
            block, head = item["at"]
            seen = product(halves(item["pair"][span:, :span]), item["solved"])
            local_ref[head, block] = seen[:, :size] + item["mixed"][span:]
            map_ref[head, block] = item["lead_query"] + seen[:, size:]
            carried = product(item["solved"], halves(item["tail_write"]), ((0,), (0,)))
            carry_ref[head, block] = carried[size:] + square * item["ended"]
            add_ref[head, block] = carried[:size] + product(
                halves(item["value"]), halves(item["tail_key"]), ((0,), (0,))
            )
        return 0

    lax.fori_loop(0, blocks // group, step, 0)

    states = [begin_ref[head] for head in range(heads)]
    for block in range(blocks):
        rows = pl.ds(block * span, span)
        gate = proj_ref[rows, 4 * wide : 5 * wide].astype(f32)
        pieces = []
        for head in range(heads):
            at = slice(head * size, (head + 1) * size)
            state = halves(states[head])
            out = local_ref[head, block] + product(
                halves(map_ref[head, block]), state, ((1,), (1,))
            )
            states[head] = product(state, halves(carry_ref[head, block])) + add_ref[head, block]
            centered = out - jnp.mean(out, axis=1, keepdims=True)
            variance = jnp.mean(centered * centered, axis=1, keepdims=True)
            pieces.append(centered * lax.rsqrt(variance + GROUP_FLOOR))
        grouped = jnp.concatenate(pieces, axis=1) * gain_ref[...]
        out_ref[rows, 0:wide] = (grouped * gate * jax.nn.sigmoid(gate)).astype(out_ref.dtype)

    lead_rows = conv_ref.shape[0] - length
    conv_ref[0:lead_rows, :] = jnp.zeros((lead_rows, channels), f32)
    conv_at = 5 * wide
    for block in range(blocks):
        rows = pl.ds(block * span, span)
        value = proj_ref[rows, conv_at : conv_at + channels].astype(f32)
        admit = proj_ref[rows, conv_at + channels : conv_at + 2 * channels].astype(f32)
        conv_ref[pl.ds(lead_rows + block * span, span), :] = (
            (value * jax.nn.sigmoid(admit)).astype(jnp.bfloat16).astype(f32)
        )
    for block in range(blocks):
        total = jnp.zeros((span, channels), f32)
        for place in range(kernel):
            first = lead_rows - (kernel - 1) + block * span + place
            total = total + taps_ref[place : place + 1, :] * conv_ref[pl.ds(first, span), :]
        rows = pl.ds(block * span, span)
        out_ref[rows, wide : wide + channels] = total.astype(out_ref.dtype)
        out_ref[rows, wide + channels : wide + 2 * channels] = proj_ref[
            rows, conv_at + 2 * channels : conv_at + 3 * channels
        ]


def mixer(projected, pace, base, correction, gain, taps, begin):
    length = projected.shape[0]
    heads, size, _ = begin.shape
    kernel, channels = taps.shape
    span = 64
    blocks = length // span
    group = next(n for n in (4, 3, 2, 1) if blocks % n == 0)
    lead_rows = -(-(kernel - 1) // 8) * 8
    maps = pltpu.VMEM((heads, blocks, size, size), jnp.float32)
    return pl.pallas_call(
        functools.partial(mixer_kernel, size, span, group),
        out_shape=jax.ShapeDtypeStruct((length, heads * size + 2 * channels), jnp.bfloat16),
        in_specs=[pl.BlockSpec(memory_space=pltpu.VMEM)] * 7,
        out_specs=pl.BlockSpec(memory_space=pltpu.VMEM),
        scratch_shapes=[
            pltpu.VMEM((heads, blocks, span, size), jnp.float32),
            pltpu.VMEM((heads, blocks, span, size), jnp.float32),
            maps,
            maps,
            pltpu.VMEM((lead_rows + length, channels), jnp.float32),
        ],
        compiler_params=pltpu.CompilerParams(vmem_limit_bytes=48 * 1024 * 1024),
        cost_estimate=pl.CostEstimate(
            flops=60_000_000_000, bytes_accessed=4_000_000, transcendentals=0
        ),
        name="mixer",
    )(projected, pace, base, correction, gain, taps, begin)


def own_part(array, axis, count, dim):
    part = array.shape[dim] // count
    return lax.dynamic_slice_in_dim(array, lax.axis_index(axis) * part, part, dim)


def whole_sequence_body(
    tokens,
    decay_pace,
    start_state,
    norm_gain,
    conv_value,
    conv_admit,
    conv_gate,
    state_query,
    state_key,
    state_value,
    state_decay,
    state_gate,
    conv_taps,
    conv_gain,
    point_weight,
    decay_base,
    correction,
    group_gain,
    output_conv,
    output_state,
):
    along = lax.axis_size("sp")
    across = lax.axis_size("fs")
    groups = lax.axis_size("tp")
    width = tokens.shape[-1]
    rows = tokens.reshape(-1, width)
    depth = conv_value.shape[0]

    shards = (
        state_query,
        state_key,
        state_value,
        state_decay,
        state_gate,
        conv_value,
        conv_admit,
        conv_gate,
    )
    parted = jnp.concatenate(
        [shard.reshape(depth, along, -1).transpose(1, 0, 2) for shard in shards], axis=2
    )
    swapped = lax.all_to_all(parted, "sp", split_axis=0, concat_axis=0, tiled=True)
    weights = lax.all_gather(swapped, "fs", axis=0).reshape(width, -1)

    floats = rows.astype(jnp.float32)
    inverse = lax.rsqrt(jnp.mean(floats * floats, axis=1, keepdims=True) + NORM_FLOOR)
    normed = (floats * inverse * norm_gain).astype(jnp.bfloat16)
    normed = (
        normed.reshape(-1, along, across, depth).transpose(0, 2, 1, 3).reshape(rows.shape)
    )
    sequence = lax.all_gather(normed, "sp", axis=0, tiled=True)
    projected = jnp.dot(sequence, weights, preferred_element_type=jnp.float32).astype(jnp.bfloat16)
    pace = lax.all_gather(decay_pace.reshape(-1), "sp", axis=0, tiled=True)[:, None]

    channels = conv_value.shape[1]
    mixed_in = mixer(
        projected,
        pace,
        own_part(decay_base[None], "sp", along, 1),
        own_part(correction[None], "sp", along, 1),
        own_part(group_gain[None], "sp", along, 1),
        own_part(conv_taps, "sp", along, 1),
        own_part(start_state[0], "sp", along, 0),
    )
    owners = along * groups
    heads_wide = state_query.shape[1] // along
    part = channels // along
    sent = mixed_in.reshape(owners, -1, mixed_in.shape[1])
    moved = lax.all_to_all(sent, ("sp", "tp"), split_axis=0, concat_axis=0, tiled=True)
    own_rows = moved.shape[1]
    moved = moved.reshape(along, groups, own_rows, -1).transpose(2, 1, 0, 3)
    state_out = moved[..., :heads_wide].reshape(own_rows, groups, -1)
    conv_sum = (
        moved[..., heads_wide : heads_wide + part].reshape(own_rows, -1).astype(jnp.float32)
    )
    gate_conv = moved[..., heads_wide + part :].reshape(own_rows, -1).astype(jnp.float32)

    columns = output_conv.shape[1]
    local_rows = output_conv.shape[0] + output_state.shape[0]
    gain_rows = conv_gain.astype(jnp.bfloat16).reshape(-1, columns)
    spare = -gain_rows.shape[0] % 16
    joined = lax.all_gather(
        jnp.concatenate(
            [
                output_conv,
                output_state,
                gain_rows,
                jnp.zeros((spare, columns), jnp.bfloat16),
            ],
            axis=0,
        ),
        "tp",
        axis=0,
    )
    whole_gain = (
        joined[:, local_rows : local_rows + gain_rows.shape[0]].reshape(-1).astype(jnp.float32)
    )
    output_rows = joined[:, :local_rows].reshape(-1, columns)
    output_weights = lax.all_gather(output_rows, ("sp", "fs"), axis=1, tiled=True)

    mean = jnp.mean(conv_sum, axis=1, keepdims=True)
    spread = jnp.mean(conv_sum * conv_sum, axis=1, keepdims=True) - mean * mean
    shaped = jax.nn.silu(
        (conv_sum - mean) * lax.rsqrt(spread + CHANNEL_FLOOR) * whole_gain
    ).astype(jnp.bfloat16)
    pointwise = jnp.dot(shaped, point_weight, preferred_element_type=jnp.float32)
    conv_out = (pointwise * jax.nn.silu(gate_conv)).astype(jnp.bfloat16)
    joined_rows = jnp.concatenate(
        [conv_out.reshape(own_rows, groups, -1), state_out], axis=2
    ).reshape(own_rows, -1)
    mixed = jnp.dot(joined_rows, output_weights, preferred_element_type=jnp.float32)
    return mixed.astype(jnp.bfloat16).reshape(1, -1, width)


def dispatch(*arrays):
    along = lax.axis_size("sp")
    tokens, start_state, conv_value, conv_gain, output_conv = (
        arrays[0],
        arrays[2],
        arrays[4],
        arrays[13],
        arrays[18],
    )
    fits = (
        start_state.shape[1] % along == 0
        and (conv_value.shape[1] // along) % 64 == 0
        and conv_gain.shape[0] % output_conv.shape[1] == 0
        and (tokens.shape[1] * along) % 64 == 0
    )
    return (whole_sequence_body if fits else body)(*arrays)


def solution(mesh):
    return jax.shard_map(
        dispatch,
        mesh=mesh,
        in_specs=(
            P("fs", "sp", None),
            P("fs", "sp"),
            P("fs", "tp", None, None),
            P(),
            P(("sp", "fs"), "tp"),
            P(("sp", "fs"), "tp"),
            P(("sp", "fs"), "tp"),
            P(("sp", "fs"), "tp"),
            P(("sp", "fs"), "tp"),
            P(("sp", "fs"), "tp"),
            P(("sp", "fs"), "tp"),
            P(("sp", "fs"), "tp"),
            P(None, "tp"),
            P("tp"),
            P(),
            P("tp"),
            P("tp"),
            P("tp"),
            P("tp", ("sp", "fs")),
            P("tp", ("sp", "fs")),
        ),
        out_specs=P("fs", ("sp", "tp"), None),
        check_vma=False,
    )
```

```python
import functools

import jax
import jax.numpy as jnp
from jax import lax
from jax.experimental import pallas as pl
from jax.experimental.pallas import tpu as pltpu
from jax.sharding import PartitionSpec as P

NORM_FLOOR = 0.1
CHANNEL_FLOOR = 0.1
GROUP_FLOOR = 1.0


def passed_along(value, axis, steps):
    count = lax.axis_size(axis)
    leading, last = (max(0, -steps), min(count, count - steps))
    return lax.ppermute(value, axis, [(source, source + steps) for source in range(leading, last)])


def entering_2(value, axis, join, neutral):
    place = lax.axis_index(axis)
    gathered = jax.tree.map(
        lambda a, kind: lax.all_gather(a.astype(kind), axis),
        value,
        jax.tree.map(lambda a: jnp.bfloat16 if a.dtype == jnp.float32 else a.dtype, value),
    )
    state = jax.tree.map(lambda a, e: jnp.zeros_like(a) + jnp.asarray(e, a.dtype), value, neutral)

    def one(lap, state):
        return join(
            state,
            jax.tree.map(
                lambda a, own: lax.dynamic_index_in_dim(a, lap, 0, False).astype(own.dtype),
                gathered,
                value,
            ),
        )

    return lax.fori_loop(0, place, one, state)


def apply_map(matrix, right):
    return jnp.einsum("hbti,hbic->hbtc", matrix, right, precision=lax.Precision.HIGHEST)


def pair_terms(left, right, mask):
    return jnp.einsum("hbtc,hbic->hbti", left, right, precision=lax.Precision.HIGHEST) * mask


def compose(earlier, later):
    first = jnp.matmul(earlier[0], later[0], precision=lax.Precision.HIGHEST)
    second = jnp.matmul(earlier[1], later[0], precision=lax.Precision.HIGHEST) + later[1]
    return (first, second)


def block_terms(query, keys, values, unit, write, log_keep):
    size = query.shape[-1]
    span = query.shape[2]
    total_log = jnp.cumsum(log_keep, axis=2)
    before_log = total_log - log_keep
    last_log = total_log[:, :, span - 1 :, :]
    lead_remove = -unit * jnp.exp(before_log)
    lead_query = query * jnp.exp(total_log)
    back_write = write * jnp.exp(-total_log)
    back_key = keys * jnp.exp(-total_log)
    places = jnp.arange(span)
    strict = (places[:, None] > places[None, :]).astype(jnp.float32)
    weak = (places[:, None] >= places[None, :]).astype(jnp.float32)
    remove_write = pair_terms(lead_remove, back_write, strict)
    remove_key = pair_terms(lead_remove, back_key, strict)
    query_write = pair_terms(lead_query, back_write, weak)
    query_key = pair_terms(lead_query, back_key, weak)
    right_side = jnp.concatenate([apply_map(remove_key, values), lead_remove], axis=-1)
    system = jnp.eye(span, dtype=jnp.float32) - remove_write
    solved = jax.scipy.linalg.solve_triangular(system, right_side, lower=True, unit_diagonal=True)
    own_part = solved[..., :size]
    start_part = solved[..., size:]
    local_out = apply_map(query_write, own_part) + apply_map(query_key, values)
    start_map = lead_query + apply_map(query_write, start_part)
    tail_write = write * jnp.exp(last_log - total_log)
    tail_key = keys * jnp.exp(last_log - total_log)
    carry_map = jnp.einsum(
        "hbtk,hbtj->hbkj", start_part, tail_write, precision=lax.Precision.HIGHEST
    ) + jnp.eye(size, dtype=jnp.float32) * jnp.exp(last_log)
    carry_add = jnp.einsum(
        "hbtv,hbtj->hbvj", own_part, tail_write, precision=lax.Precision.HIGHEST
    ) + jnp.einsum("hbtv,hbtj->hbvj", values, tail_key, precision=lax.Precision.HIGHEST)
    return (local_out, start_map, carry_map, carry_add)


def body(
    tokens,
    decay_pace,
    start_state,
    norm_gain,
    conv_value,
    conv_admit,
    conv_gate,
    state_query,
    state_key,
    state_value,
    state_decay,
    state_gate,
    conv_taps,
    conv_gain,
    point_weight,
    decay_base,
    correction,
    group_gain,
    output_conv,
    output_state,
):
    width = tokens.shape[-1]
    rows = tokens.reshape(-1, width)
    length = rows.shape[0]
    floats = rows.astype(jnp.float32)
    inverse = lax.rsqrt(jnp.mean(floats * floats, axis=1, keepdims=True) + NORM_FLOOR)
    normed = (floats * inverse * norm_gain).astype(jnp.bfloat16)
    shards = (
        conv_value,
        conv_admit,
        conv_gate,
        state_query,
        state_key,
        state_value,
        state_decay,
        state_gate,
    )
    stacked = jnp.concatenate(shards, axis=1)
    projected = jnp.dot(
        normed,
        lax.all_gather(stacked, ("sp", "fs"), axis=0, tiled=True),
        preferred_element_type=jnp.float32,
    ).astype(jnp.bfloat16)
    pieces = []
    offset = 0
    for shard in shards:
        pieces.append(projected[:, offset : offset + shard.shape[1]].astype(jnp.float32))
        offset = offset + shard.shape[1]
    value, admit, gate_conv, query, keys, values, decay_in, gate_state = pieces
    channels = value.shape[1]
    kernel = conv_taps.shape[0]
    conv_input = (value * jax.nn.sigmoid(admit)).astype(jnp.bfloat16)
    earlier = passed_along(conv_input[length - (kernel - 1) :], "sp", 1)
    padded = jnp.concatenate([earlier, conv_input], axis=0).astype(jnp.float32)
    conv_sum = jnp.zeros((length, channels), jnp.float32)
    for place in range(kernel):
        conv_sum = conv_sum + conv_taps[place] * padded[place : place + length]
    local_point = lax.dynamic_slice_in_dim(
        point_weight, lax.axis_index("tp") * channels, channels, 1
    )
    whole_sum, whole_gain = (
        lax.all_gather(conv_sum.astype(jnp.bfloat16), "tp", axis=1, tiled=True).astype(
            conv_sum.dtype
        ),
        lax.all_gather(conv_gain.astype(jnp.bfloat16), "tp", axis=0, tiled=True).astype(
            conv_gain.dtype
        ),
    )
    mean = jnp.mean(whole_sum, axis=1, keepdims=True)
    spread = jnp.mean(whole_sum * whole_sum, axis=1, keepdims=True) - mean * mean
    shaped = jax.nn.silu(
        (whole_sum - mean) * lax.rsqrt(spread + CHANNEL_FLOOR) * whole_gain
    ).astype(jnp.bfloat16)
    pointwise = jnp.dot(shaped, local_point, preferred_element_type=jnp.float32)
    conv_out = (pointwise * jax.nn.silu(gate_conv)).astype(jnp.bfloat16)
    size = start_state.shape[-1]
    heads = query.shape[1] // size
    span = min(64, length)
    blocks = length // span
    log_keep = -jnp.exp(decay_base + jnp.tanh(decay_in)) * decay_pace.reshape(-1)[:, None]
    key_heads = keys.reshape(length, heads, size)
    unit = key_heads * lax.rsqrt(
        jnp.maximum(jnp.sum(key_heads * key_heads, axis=-1, keepdims=True), 1.0)
    )
    write = unit * correction.reshape(heads, size)

    def arrange(array):
        return array.reshape(blocks, span, heads, size).transpose(2, 0, 1, 3)

    local_out, start_map, carry_map, carry_add = block_terms(
        arrange(query),
        arrange(keys),
        arrange(values),
        arrange(unit),
        arrange(write),
        arrange(log_keep),
    )
    identity = (
        jnp.broadcast_to(jnp.eye(size, dtype=jnp.float32), (heads, size, size)),
        jnp.zeros((heads, size, size), jnp.float32),
    )

    def along(carried, block_pair):
        return (compose(carried, block_pair), carried)

    device_pair, prefixes = lax.scan(
        along, identity, (jnp.moveaxis(carry_map, 1, 0), jnp.moveaxis(carry_add, 1, 0))
    )
    prior_map, prior_add = entering_2(device_pair, "sp", compose, identity)
    begin = start_state.reshape(heads, size, size)
    entering = jnp.matmul(begin, prior_map, precision=lax.Precision.HIGHEST) + prior_add
    block_starts = (
        jnp.matmul(entering[None], prefixes[0], precision=lax.Precision.HIGHEST) + prefixes[1]
    )
    block_starts = jnp.moveaxis(block_starts, 0, 1)
    outputs = local_out + jnp.einsum(
        "hbtk,hbvk->hbtv", start_map, block_starts, precision=lax.Precision.HIGHEST
    )
    outputs = outputs.transpose(1, 2, 0, 3).reshape(length, heads, size)
    centered = outputs - jnp.mean(outputs, axis=-1, keepdims=True)
    variance = jnp.mean(centered * centered, axis=-1, keepdims=True)
    grouped = centered * lax.rsqrt(variance + GROUP_FLOOR) * group_gain.reshape(heads, size)
    state_out = (grouped.reshape(length, heads * size) * jax.nn.silu(gate_state)).astype(
        jnp.bfloat16
    )
    local_mix = jnp.concatenate([conv_out, state_out], axis=1)
    moved = lax.all_to_all(local_mix, "tp", split_axis=0, concat_axis=1, tiled=True)
    conv_rows, state_rows = (
        lax.all_gather(output_conv, "tp", axis=0, tiled=True),
        lax.all_gather(output_state, "tp", axis=0, tiled=True),
    )
    groups = lax.axis_size("tp")
    joined = jnp.concatenate(
        [conv_rows.reshape(groups, channels, -1), state_rows.reshape(groups, heads * size, -1)],
        axis=1,
    )
    joined = joined.reshape(groups * (channels + heads * size), -1)
    mixed = jnp.dot(
        moved,
        lax.all_gather(joined, ("sp", "fs"), axis=1, tiled=True),
        preferred_element_type=jnp.float32,
    )
    return mixed.astype(jnp.bfloat16).reshape(1, -1, width)


def halves(array):
    high = array.astype(jnp.bfloat16)
    low = (array - high.astype(jnp.float32)).astype(jnp.bfloat16)
    return (high, low)


def product(left, right, dims=((1,), (0,))):
    def one(a, b):
        return lax.dot_general(a, b, (dims, ((), ())), preferred_element_type=jnp.float32)

    return one(left[0], right[0]) + (one(left[0], right[1]) + one(left[1], right[0]))


def mixer_kernel(
    size,
    span,
    group,
    proj_ref,
    pace_ref,
    base_ref,
    correction_ref,
    gain_ref,
    taps_ref,
    begin_ref,
    out_ref,
    local_ref,
    map_ref,
    carry_ref,
    add_ref,
    conv_ref,
):
    length = proj_ref.shape[0]
    heads = begin_ref.shape[0]
    wide = heads * size
    blocks = length // span
    kernel, channels = taps_ref.shape
    f32 = jnp.float32
    row = lax.broadcasted_iota(jnp.int32, (span, span), 0)
    col = lax.broadcasted_iota(jnp.int32, (span, span), 1)
    strict = (row > col).astype(f32)
    weak = (row >= col).astype(f32)
    masks = jnp.concatenate(
        [jnp.concatenate([strict, strict], axis=1), jnp.concatenate([weak, weak], axis=1)], axis=0
    )
    eye = (row == col).astype(f32)
    square = (
        lax.broadcasted_iota(jnp.int32, (size, size), 0)
        == lax.broadcasted_iota(jnp.int32, (size, size), 1)
    ).astype(f32)
    least = min(8, span)
    same = (row // least == col // least).astype(f32)
    merges = []
    width = least
    while width < span:
        merges.append(
            ((row // (2 * width) == col // (2 * width)) & (row // width != col // width)).astype(f32)
        )
        width = 2 * width
    weak_bf = weak.astype(jnp.bfloat16)

    def step(turn, _):
        items = []
        for part in range(group):
            block = turn * group + part
            rows = pl.ds(pl.multiple_of(block * span, span), span)
            query = proj_ref[rows, 0:wide].astype(f32)
            keys = proj_ref[rows, wide : 2 * wide].astype(f32)
            values = proj_ref[rows, 2 * wide : 3 * wide].astype(f32)
            decay_in = proj_ref[rows, 3 * wide : 4 * wide].astype(f32)
            log_keep = -jnp.exp(base_ref[...] + jnp.tanh(decay_in)) * pace_ref[rows, :]
            high = log_keep.astype(jnp.bfloat16)
            rest = log_keep - high.astype(f32)
            mid = rest.astype(jnp.bfloat16)
            low = (rest - mid.astype(f32)).astype(jnp.bfloat16)
            total = (
                jnp.dot(weak_bf, high, preferred_element_type=f32)
                + jnp.dot(weak_bf, mid, preferred_element_type=f32)
                + jnp.dot(weak_bf, low, preferred_element_type=f32)
            )
            last = total[span - 1 : span, :]
            lead = jnp.exp(total - log_keep)
            grown = jnp.exp(total)
            back = jnp.exp(-total)
            tail = jnp.exp(last - total)
            ended = jnp.exp(last)
            for head in range(heads):
                at = slice(head * size, (head + 1) * size)
                key = keys[:, at]
                unit = key * lax.rsqrt(
                    jnp.maximum(jnp.sum(key * key, axis=1, keepdims=True), 1.0)
                )
                write = unit * correction_ref[:, at]
                lead_remove = -unit * lead[:, at]
                lead_query = query[:, at] * grown[:, at]
                items.append(
                    dict(
                        at=(block, head),
                        value=values[:, at],
                        lead_remove=lead_remove,
                        lead_query=lead_query,
                        left=jnp.concatenate([lead_remove, lead_query], axis=0),
                        right=jnp.concatenate([write * back[:, at], key * back[:, at]], axis=0),
                        tail_write=write * tail[:, at],
                        tail_key=key * tail[:, at],
                        ended=ended[:, at],
                    )
                )
        for item in items:
            item["pair"] = (
                product(halves(item["left"]), halves(item["right"]), ((1,), (1,))) * masks
            )
        for item in items:
            item["system"] = item["pair"][:span, :span]
            item["power"] = halves(item["system"] * same)
            item["inverse"] = eye + item["system"] * same
        width = 2
        while width < least:
            for item in items:
                item["power"] = halves(product(item["power"], item["power"]))
            for item in items:
                item["inverse"] = item["inverse"] + product(
                    halves(item["inverse"]), item["power"]
                )
            width = 2 * width
        for item in items:
            padded = jnp.concatenate([jnp.zeros_like(item["value"]), item["value"]], axis=0)
            item["mixed"] = product(halves(item["pair"]), halves(padded))
        for merge in merges:
            for item in items:
                item["inside"] = halves(item["inverse"])
                item["next"] = halves(product(halves(item["system"] * merge), item["inside"]))
            for item in items:
                item["inverse"] = item["inverse"] + product(item["inside"], item["next"])
        for item in items:
            right_side = jnp.concatenate([item["mixed"][:span], item["lead_remove"]], axis=1)
            item["solved"] = halves(product(halves(item["inverse"]), halves(right_side)))
        for item in items:
            block, head = item["at"]
            seen = product(halves(item["pair"][span:, :span]), item["solved"])
            local_ref[head, block] = seen[:, :size] + item["mixed"][span:]
            map_ref[head, block] = item["lead_query"] + seen[:, size:]
            carried = product(item["solved"], halves(item["tail_write"]), ((0,), (0,)))
            carry_ref[head, block] = carried[size:] + square * item["ended"]
            add_ref[head, block] = carried[:size] + product(
                halves(item["value"]), halves(item["tail_key"]), ((0,), (0,))
            )
        return 0

    lax.fori_loop(0, blocks // group, step, 0)

    states = [begin_ref[head] for head in range(heads)]
    for block in range(blocks):
        rows = pl.ds(block * span, span)
        gate = proj_ref[rows, 4 * wide : 5 * wide].astype(f32)
        pieces = []
        for head in range(heads):
            at = slice(head * size, (head + 1) * size)
            state = halves(states[head])
            out = local_ref[head, block] + product(
                halves(map_ref[head, block]), state, ((1,), (1,))
            )
            states[head] = product(state, halves(carry_ref[head, block])) + add_ref[head, block]
            centered = out - jnp.mean(out, axis=1, keepdims=True)
            variance = jnp.mean(centered * centered, axis=1, keepdims=True)
            pieces.append(centered * lax.rsqrt(variance + GROUP_FLOOR))
        grouped = jnp.concatenate(pieces, axis=1) * gain_ref[...]
        out_ref[rows, 0:wide] = (grouped * gate * jax.nn.sigmoid(gate)).astype(out_ref.dtype)

    lead_rows = conv_ref.shape[0] - length
    conv_ref[0:lead_rows, :] = jnp.zeros((lead_rows, channels), f32)
    conv_at = 5 * wide
    for block in range(blocks):
        rows = pl.ds(block * span, span)
        value = proj_ref[rows, conv_at : conv_at + channels].astype(f32)
        admit = proj_ref[rows, conv_at + channels : conv_at + 2 * channels].astype(f32)
        conv_ref[pl.ds(lead_rows + block * span, span), :] = (
            (value * jax.nn.sigmoid(admit)).astype(jnp.bfloat16).astype(f32)
        )
    for block in range(blocks):
        total = jnp.zeros((span, channels), f32)
        for place in range(kernel):
            first = lead_rows - (kernel - 1) + block * span + place
            total = total + taps_ref[place : place + 1, :] * conv_ref[pl.ds(first, span), :]
        rows = pl.ds(block * span, span)
        out_ref[rows, wide : wide + channels] = total.astype(out_ref.dtype)
        out_ref[rows, wide + channels : wide + 2 * channels] = proj_ref[
            rows, conv_at + 2 * channels : conv_at + 3 * channels
        ]


def mixer(projected, pace, base, correction, gain, taps, begin):
    length = projected.shape[0]
    heads, size, _ = begin.shape
    kernel, channels = taps.shape
    span = 64
    blocks = length // span
    group = next(n for n in (4, 3, 2, 1) if blocks % n == 0)
    lead_rows = -(-(kernel - 1) // 8) * 8
    maps = pltpu.VMEM((heads, blocks, size, size), jnp.float32)
    return pl.pallas_call(
        functools.partial(mixer_kernel, size, span, group),
        out_shape=jax.ShapeDtypeStruct((length, heads * size + 2 * channels), jnp.bfloat16),
        in_specs=[pl.BlockSpec(memory_space=pltpu.VMEM)] * 7,
        out_specs=pl.BlockSpec(memory_space=pltpu.VMEM),
        scratch_shapes=[
            pltpu.VMEM((heads, blocks, span, size), jnp.float32),
            pltpu.VMEM((heads, blocks, span, size), jnp.float32),
            maps,
            maps,
            pltpu.VMEM((lead_rows + length, channels), jnp.float32),
        ],
        compiler_params=pltpu.CompilerParams(vmem_limit_bytes=48 * 1024 * 1024),
        cost_estimate=pl.CostEstimate(
            flops=60_000_000_000, bytes_accessed=4_000_000, transcendentals=0
        ),
        name="mixer",
    )(projected, pace, base, correction, gain, taps, begin)


def collect_kernel(
    along,
    normed_ref,
    parted_ref,
    pace_ref,
    rows_ref,
    proj_ref,
    paces_ref,
    joined_ref,
    sequence,
    weights,
    w_send,
    w_recv,
    t_send,
    t_recv,
    p_send,
    p_recv,
    y_send,
    y_recv,
    c_send,
    c_recv,
    r_send,
    r_recv,
    x_send,
    x_recv,
    o_send,
    o_recv,
):
    place = lax.axis_index("sp")
    seat = lax.axis_index("fs")
    side = lax.axis_index("tp")
    depth = parted_ref.shape[1]
    length = normed_ref.shape[0]
    half = length // 2
    near = seat + 1 - 2 * lax.rem(seat, 2)
    far = lax.rem(seat + 2, 4)
    other = 1 - side

    def ahead(steps):
        return lax.rem(place + steps, along)

    def behind(steps):
        return lax.rem(place + along - steps, along)

    def block(sp_at, fs_at):
        return weights.at[pl.ds(pl.multiple_of((sp_at * 4 + fs_at) * depth, depth), depth)]

    def tokens_at(sp_at, side_at):
        return sequence.at[
            pl.ds(pl.multiple_of(sp_at * length + side_at * half, half), half)
        ]

    def send(source, target, send_sem, recv_sem, where):
        copy = pltpu.make_async_remote_copy(
            src_ref=source,
            dst_ref=target,
            send_sem=send_sem,
            recv_sem=recv_sem,
            device_id=where,
            device_id_type=pl.DeviceIdType.MESH,
        )
        copy.start()
        sent.append(copy)

    def arrive(target, send_sem, recv_sem, where):
        pltpu.make_async_remote_copy(
            src_ref=target,
            dst_ref=target,
            send_sem=send_sem,
            recv_sem=recv_sem,
            device_id=where,
            device_id_type=pl.DeviceIdType.MESH,
        ).wait_recv()

    sent = []
    barrier = pltpu.get_barrier_semaphore()
    partners = [{"sp": ahead(s)} for s in range(1, along)]
    partners += [{"fs": near}, {"fs": far}, {"tp": other}]
    for partner in partners:
        pl.semaphore_signal(
            barrier, inc=1, device_id=partner, device_id_type=pl.DeviceIdType.MESH
        )
    pl.semaphore_wait(barrier, len(partners))

    order = sorted(range(1, along), key=lambda s: min(s, along - s))
    own = parted_ref.at[place]
    for s in order:
        send(
            parted_ref.at[ahead(s)], block(place, seat), w_send.at[s], w_recv.at[s], {"sp": ahead(s)}
        )
    send(own, block(place, seat), y_send.at[0], y_recv.at[0], {"fs": far})
    send(own, block(place, seat), c_send.at[0], c_recv.at[0], {"fs": near})
    for s in order:
        send(pace_ref, paces_ref.at[place], p_send.at[s], p_recv.at[s], {"sp": ahead(s)})
    for s in order:
        send(
            normed_ref.at[pl.ds(pl.multiple_of(side * half, half), half)],
            tokens_at(place, side),
            t_send.at[s],
            t_recv.at[s],
            {"sp": ahead(s)},
        )
    send(rows_ref, joined_ref.at[side], o_send.at[0], o_recv.at[0], {"tp": other})

    block(place, seat)[...] = parted_ref[place]
    sequence[pl.ds(pl.multiple_of(place * length, length), length), :] = normed_ref[...]
    joined_ref[side] = rows_ref[...]
    paces_ref[place] = pace_ref[...]

    def weights_on(s):
        here = block(behind(s), seat)
        arrive(here, w_send.at[s], w_recv.at[s], {"sp": ahead(s)})
        send(here, here, y_send.at[s], y_recv.at[s], {"fs": far})
        send(here, here, c_send.at[s], c_recv.at[s], {"fs": near})

    def relay(s):
        here = block(behind(s), far)
        arrive(here, y_send.at[s], y_recv.at[s], {"fs": far})
        send(here, here, r_send.at[s], r_recv.at[s], {"fs": near})

    def tokens_on(s):
        here = tokens_at(behind(s), side)
        arrive(here, t_send.at[s], t_recv.at[s], {"sp": ahead(s)})
        send(here, here, x_send.at[s], x_recv.at[s], {"tp": other})

    for s in order[:2]:
        weights_on(s)
    relay(0)
    for s in order[2:]:
        weights_on(s)
    for at, s in enumerate(order):
        relay(s)
        tokens_on(s)

    for s in [0] + order:
        arrive(block(behind(s), near), c_send.at[s], c_recv.at[s], {"fs": near})
        beyond = lax.rem(near + 2, 4)
        arrive(block(behind(s), beyond), r_send.at[s], r_recv.at[s], {"fs": near})
    for s in order:
        arrive(tokens_at(behind(s), other), x_send.at[s], x_recv.at[s], {"tp": other})
        arrive(paces_ref.at[behind(s)], p_send.at[s], p_recv.at[s], {"sp": ahead(s)})
    arrive(joined_ref.at[other], o_send.at[0], o_recv.at[0], {"tp": other})
    for copy in sent:
        copy.wait_send()

    total = sequence.shape[0]
    tile = next(n for n in (256, 192, 128, 96, 64, 32, 16) if total % n == 0)

    def multiply(turn, _):
        at = pl.ds(pl.multiple_of(turn * tile, tile), tile)
        proj_ref[at, :] = jnp.dot(
            sequence[at, :], weights[...], preferred_element_type=jnp.float32
        ).astype(proj_ref.dtype)
        return 0

    lax.fori_loop(0, total // tile, multiply, 0)


def collect(normed, parted, pace, rows):
    along = parted.shape[0]
    length, width = normed.shape
    columns = parted.shape[2]
    pair = pltpu.SemaphoreType.DMA((along,))
    single = pltpu.SemaphoreType.DMA((1,))
    return pl.pallas_call(
        functools.partial(collect_kernel, along),
        out_shape=(
            jax.ShapeDtypeStruct((along * length, columns), jnp.bfloat16),
            jax.ShapeDtypeStruct((along,) + pace.shape, pace.dtype),
            jax.ShapeDtypeStruct((2,) + rows.shape, rows.dtype),
        ),
        in_specs=[pl.BlockSpec(memory_space=pltpu.VMEM)] * 4,
        out_specs=(pl.BlockSpec(memory_space=pltpu.VMEM),) * 3,
        scratch_shapes=[
            pltpu.VMEM((along * length, width), jnp.bfloat16),
            pltpu.VMEM((width, columns), jnp.bfloat16),
        ]
        + [pair] * 14
        + [single] * 2,
        compiler_params=pltpu.CompilerParams(
            collective_id=0, has_side_effects=True, vmem_limit_bytes=48 * 1024 * 1024
        ),
        cost_estimate=pl.CostEstimate(
            flops=60_000_000_000, bytes_accessed=8_000_000, transcendentals=0
        ),
        name="collect",
    )(normed, parted, pace, rows)


def own_part(array, axis, count, dim):
    part = array.shape[dim] // count
    return lax.dynamic_slice_in_dim(array, lax.axis_index(axis) * part, part, dim)


def whole_sequence_body(
    tokens,
    decay_pace,
    start_state,
    norm_gain,
    conv_value,
    conv_admit,
    conv_gate,
    state_query,
    state_key,
    state_value,
    state_decay,
    state_gate,
    conv_taps,
    conv_gain,
    point_weight,
    decay_base,
    correction,
    group_gain,
    output_conv,
    output_state,
):
    along = lax.axis_size("sp")
    groups = lax.axis_size("tp")
    width = tokens.shape[-1]
    rows = tokens.reshape(-1, width)
    depth = conv_value.shape[0]

    shards = (
        state_query,
        state_key,
        state_value,
        state_decay,
        state_gate,
        conv_value,
        conv_admit,
        conv_gate,
    )
    parted = jnp.concatenate(
        [shard.reshape(depth, along, -1).transpose(1, 0, 2) for shard in shards], axis=2
    )
    floats = rows.astype(jnp.float32)
    inverse = lax.rsqrt(jnp.mean(floats * floats, axis=1, keepdims=True) + NORM_FLOOR)
    normed = (floats * inverse * norm_gain).astype(jnp.bfloat16)
    columns = output_conv.shape[1]
    local_rows = output_conv.shape[0] + output_state.shape[0]
    gain_rows = conv_gain.astype(jnp.bfloat16).reshape(-1, columns)
    spare = -gain_rows.shape[0] % 16
    sent_rows = jnp.concatenate(
        [output_conv, output_state, gain_rows, jnp.zeros((spare, columns), jnp.bfloat16)], axis=0
    )
    span = rows.shape[0]
    lanes = -(-span // 128) * 128
    sent_pace = jnp.broadcast_to(
        jnp.pad(decay_pace.reshape(1, -1), ((0, 0), (0, lanes - span))), (8, lanes)
    )
    projected, paces, joined = collect(normed, parted, sent_pace, sent_rows)
    pace = paces[:, 0, :span].reshape(-1, 1)

    channels = conv_value.shape[1]
    mixed_in = mixer(
        projected,
        pace,
        own_part(decay_base[None], "sp", along, 1),
        own_part(correction[None], "sp", along, 1),
        own_part(group_gain[None], "sp", along, 1),
        own_part(conv_taps, "sp", along, 1),
        own_part(start_state[0], "sp", along, 0),
    )
    owners = along * groups
    heads_wide = state_query.shape[1] // along
    part = channels // along
    sent = mixed_in.reshape(owners, -1, mixed_in.shape[1])
    moved = lax.all_to_all(sent, ("sp", "tp"), split_axis=0, concat_axis=0, tiled=True)
    own_rows = moved.shape[1]
    moved = moved.reshape(along, groups, own_rows, -1).transpose(2, 1, 0, 3)
    state_out = moved[..., :heads_wide].reshape(own_rows, groups, -1)
    conv_sum = (
        moved[..., heads_wide : heads_wide + part].reshape(own_rows, -1).astype(jnp.float32)
    )
    gate_conv = moved[..., heads_wide + part :].reshape(own_rows, -1).astype(jnp.float32)

    whole_gain = (
        joined[:, local_rows : local_rows + gain_rows.shape[0]].reshape(-1).astype(jnp.float32)
    )
    output_rows = joined[:, :local_rows].reshape(-1, columns)
    output_weights = lax.all_gather(output_rows, ("sp", "fs"), axis=1, tiled=True)

    mean = jnp.mean(conv_sum, axis=1, keepdims=True)
    spread = jnp.mean(conv_sum * conv_sum, axis=1, keepdims=True) - mean * mean
    shaped = jax.nn.silu(
        (conv_sum - mean) * lax.rsqrt(spread + CHANNEL_FLOOR) * whole_gain
    ).astype(jnp.bfloat16)
    pointwise = jnp.dot(shaped, point_weight, preferred_element_type=jnp.float32)
    conv_out = (pointwise * jax.nn.silu(gate_conv)).astype(jnp.bfloat16)
    joined_rows = jnp.concatenate(
        [conv_out.reshape(own_rows, groups, -1), state_out], axis=2
    ).reshape(own_rows, -1)
    mixed = jnp.dot(joined_rows, output_weights, preferred_element_type=jnp.float32)
    return mixed.astype(jnp.bfloat16).reshape(1, -1, width)


def dispatch(*arrays):
    along = lax.axis_size("sp")
    tokens, start_state, conv_value, conv_gain, output_conv = (
        arrays[0],
        arrays[2],
        arrays[4],
        arrays[13],
        arrays[18],
    )
    fits = (
        along > 2
        and lax.axis_size("fs") == 4
        and lax.axis_size("tp") == 2
        and tokens.shape[1] % 32 == 0
        and start_state.shape[1] % along == 0
        and (conv_value.shape[1] // along) % 64 == 0
        and conv_gain.shape[0] % output_conv.shape[1] == 0
        and (tokens.shape[1] * along) % 64 == 0
    )
    return (whole_sequence_body if fits else body)(*arrays)


def solution(mesh):
    return jax.shard_map(
        dispatch,
        mesh=mesh,
        in_specs=(
            P("fs", "sp", None),
            P("fs", "sp"),
            P("fs", "tp", None, None),
            P(),
            P(("sp", "fs"), "tp"),
            P(("sp", "fs"), "tp"),
            P(("sp", "fs"), "tp"),
            P(("sp", "fs"), "tp"),
            P(("sp", "fs"), "tp"),
            P(("sp", "fs"), "tp"),
            P(("sp", "fs"), "tp"),
            P(("sp", "fs"), "tp"),
            P(None, "tp"),
            P("tp"),
            P(),
            P("tp"),
            P("tp"),
            P("tp"),
            P("tp", ("sp", "fs")),
            P("tp", ("sp", "fs")),
        ),
        out_specs=P("fs", ("sp", "tp"), None),
        check_vma=False,
    )
```

```python
import functools

import jax
import jax.numpy as jnp
from jax import lax
from jax.experimental import pallas as pl
from jax.experimental.pallas import tpu as pltpu
from jax.sharding import PartitionSpec as P

NORM_FLOOR = 0.1
CHANNEL_FLOOR = 0.1
GROUP_FLOOR = 1.0


def passed_along(value, axis, steps):
    count = lax.axis_size(axis)
    leading, last = (max(0, -steps), min(count, count - steps))
    return lax.ppermute(value, axis, [(source, source + steps) for source in range(leading, last)])


def entering_2(value, axis, join, neutral):
    place = lax.axis_index(axis)
    gathered = jax.tree.map(
        lambda a, kind: lax.all_gather(a.astype(kind), axis),
        value,
        jax.tree.map(lambda a: jnp.bfloat16 if a.dtype == jnp.float32 else a.dtype, value),
    )
    state = jax.tree.map(lambda a, e: jnp.zeros_like(a) + jnp.asarray(e, a.dtype), value, neutral)

    def one(lap, state):
        return join(
            state,
            jax.tree.map(
                lambda a, own: lax.dynamic_index_in_dim(a, lap, 0, False).astype(own.dtype),
                gathered,
                value,
            ),
        )

    return lax.fori_loop(0, place, one, state)


def apply_map(matrix, right):
    return jnp.einsum("hbti,hbic->hbtc", matrix, right, precision=lax.Precision.HIGHEST)


def pair_terms(left, right, mask):
    return jnp.einsum("hbtc,hbic->hbti", left, right, precision=lax.Precision.HIGHEST) * mask


def compose(earlier, later):
    first = jnp.matmul(earlier[0], later[0], precision=lax.Precision.HIGHEST)
    second = jnp.matmul(earlier[1], later[0], precision=lax.Precision.HIGHEST) + later[1]
    return (first, second)


def block_terms(query, keys, values, unit, write, log_keep):
    size = query.shape[-1]
    span = query.shape[2]
    total_log = jnp.cumsum(log_keep, axis=2)
    before_log = total_log - log_keep
    last_log = total_log[:, :, span - 1 :, :]
    lead_remove = -unit * jnp.exp(before_log)
    lead_query = query * jnp.exp(total_log)
    back_write = write * jnp.exp(-total_log)
    back_key = keys * jnp.exp(-total_log)
    places = jnp.arange(span)
    strict = (places[:, None] > places[None, :]).astype(jnp.float32)
    weak = (places[:, None] >= places[None, :]).astype(jnp.float32)
    remove_write = pair_terms(lead_remove, back_write, strict)
    remove_key = pair_terms(lead_remove, back_key, strict)
    query_write = pair_terms(lead_query, back_write, weak)
    query_key = pair_terms(lead_query, back_key, weak)
    right_side = jnp.concatenate([apply_map(remove_key, values), lead_remove], axis=-1)
    system = jnp.eye(span, dtype=jnp.float32) - remove_write
    solved = jax.scipy.linalg.solve_triangular(system, right_side, lower=True, unit_diagonal=True)
    own_part = solved[..., :size]
    start_part = solved[..., size:]
    local_out = apply_map(query_write, own_part) + apply_map(query_key, values)
    start_map = lead_query + apply_map(query_write, start_part)
    tail_write = write * jnp.exp(last_log - total_log)
    tail_key = keys * jnp.exp(last_log - total_log)
    carry_map = jnp.einsum(
        "hbtk,hbtj->hbkj", start_part, tail_write, precision=lax.Precision.HIGHEST
    ) + jnp.eye(size, dtype=jnp.float32) * jnp.exp(last_log)
    carry_add = jnp.einsum(
        "hbtv,hbtj->hbvj", own_part, tail_write, precision=lax.Precision.HIGHEST
    ) + jnp.einsum("hbtv,hbtj->hbvj", values, tail_key, precision=lax.Precision.HIGHEST)
    return (local_out, start_map, carry_map, carry_add)


def body(
    tokens,
    decay_pace,
    start_state,
    norm_gain,
    conv_value,
    conv_admit,
    conv_gate,
    state_query,
    state_key,
    state_value,
    state_decay,
    state_gate,
    conv_taps,
    conv_gain,
    point_weight,
    decay_base,
    correction,
    group_gain,
    output_conv,
    output_state,
):
    width = tokens.shape[-1]
    rows = tokens.reshape(-1, width)
    length = rows.shape[0]
    floats = rows.astype(jnp.float32)
    inverse = lax.rsqrt(jnp.mean(floats * floats, axis=1, keepdims=True) + NORM_FLOOR)
    normed = (floats * inverse * norm_gain).astype(jnp.bfloat16)
    shards = (
        conv_value,
        conv_admit,
        conv_gate,
        state_query,
        state_key,
        state_value,
        state_decay,
        state_gate,
    )
    stacked = jnp.concatenate(shards, axis=1)
    projected = jnp.dot(
        normed,
        lax.all_gather(stacked, ("sp", "fs"), axis=0, tiled=True),
        preferred_element_type=jnp.float32,
    ).astype(jnp.bfloat16)
    pieces = []
    offset = 0
    for shard in shards:
        pieces.append(projected[:, offset : offset + shard.shape[1]].astype(jnp.float32))
        offset = offset + shard.shape[1]
    value, admit, gate_conv, query, keys, values, decay_in, gate_state = pieces
    channels = value.shape[1]
    kernel = conv_taps.shape[0]
    conv_input = (value * jax.nn.sigmoid(admit)).astype(jnp.bfloat16)
    earlier = passed_along(conv_input[length - (kernel - 1) :], "sp", 1)
    padded = jnp.concatenate([earlier, conv_input], axis=0).astype(jnp.float32)
    conv_sum = jnp.zeros((length, channels), jnp.float32)
    for place in range(kernel):
        conv_sum = conv_sum + conv_taps[place] * padded[place : place + length]
    local_point = lax.dynamic_slice_in_dim(
        point_weight, lax.axis_index("tp") * channels, channels, 1
    )
    whole_sum, whole_gain = (
        lax.all_gather(conv_sum.astype(jnp.bfloat16), "tp", axis=1, tiled=True).astype(
            conv_sum.dtype
        ),
        lax.all_gather(conv_gain.astype(jnp.bfloat16), "tp", axis=0, tiled=True).astype(
            conv_gain.dtype
        ),
    )
    mean = jnp.mean(whole_sum, axis=1, keepdims=True)
    spread = jnp.mean(whole_sum * whole_sum, axis=1, keepdims=True) - mean * mean
    shaped = jax.nn.silu(
        (whole_sum - mean) * lax.rsqrt(spread + CHANNEL_FLOOR) * whole_gain
    ).astype(jnp.bfloat16)
    pointwise = jnp.dot(shaped, local_point, preferred_element_type=jnp.float32)
    conv_out = (pointwise * jax.nn.silu(gate_conv)).astype(jnp.bfloat16)
    size = start_state.shape[-1]
    heads = query.shape[1] // size
    span = min(64, length)
    blocks = length // span
    log_keep = -jnp.exp(decay_base + jnp.tanh(decay_in)) * decay_pace.reshape(-1)[:, None]
    key_heads = keys.reshape(length, heads, size)
    unit = key_heads * lax.rsqrt(
        jnp.maximum(jnp.sum(key_heads * key_heads, axis=-1, keepdims=True), 1.0)
    )
    write = unit * correction.reshape(heads, size)

    def arrange(array):
        return array.reshape(blocks, span, heads, size).transpose(2, 0, 1, 3)

    local_out, start_map, carry_map, carry_add = block_terms(
        arrange(query),
        arrange(keys),
        arrange(values),
        arrange(unit),
        arrange(write),
        arrange(log_keep),
    )
    identity = (
        jnp.broadcast_to(jnp.eye(size, dtype=jnp.float32), (heads, size, size)),
        jnp.zeros((heads, size, size), jnp.float32),
    )

    def along(carried, block_pair):
        return (compose(carried, block_pair), carried)

    device_pair, prefixes = lax.scan(
        along, identity, (jnp.moveaxis(carry_map, 1, 0), jnp.moveaxis(carry_add, 1, 0))
    )
    prior_map, prior_add = entering_2(device_pair, "sp", compose, identity)
    begin = start_state.reshape(heads, size, size)
    entering = jnp.matmul(begin, prior_map, precision=lax.Precision.HIGHEST) + prior_add
    block_starts = (
        jnp.matmul(entering[None], prefixes[0], precision=lax.Precision.HIGHEST) + prefixes[1]
    )
    block_starts = jnp.moveaxis(block_starts, 0, 1)
    outputs = local_out + jnp.einsum(
        "hbtk,hbvk->hbtv", start_map, block_starts, precision=lax.Precision.HIGHEST
    )
    outputs = outputs.transpose(1, 2, 0, 3).reshape(length, heads, size)
    centered = outputs - jnp.mean(outputs, axis=-1, keepdims=True)
    variance = jnp.mean(centered * centered, axis=-1, keepdims=True)
    grouped = centered * lax.rsqrt(variance + GROUP_FLOOR) * group_gain.reshape(heads, size)
    state_out = (grouped.reshape(length, heads * size) * jax.nn.silu(gate_state)).astype(
        jnp.bfloat16
    )
    local_mix = jnp.concatenate([conv_out, state_out], axis=1)
    moved = lax.all_to_all(local_mix, "tp", split_axis=0, concat_axis=1, tiled=True)
    conv_rows, state_rows = (
        lax.all_gather(output_conv, "tp", axis=0, tiled=True),
        lax.all_gather(output_state, "tp", axis=0, tiled=True),
    )
    groups = lax.axis_size("tp")
    joined = jnp.concatenate(
        [conv_rows.reshape(groups, channels, -1), state_rows.reshape(groups, heads * size, -1)],
        axis=1,
    )
    joined = joined.reshape(groups * (channels + heads * size), -1)
    mixed = jnp.dot(
        moved,
        lax.all_gather(joined, ("sp", "fs"), axis=1, tiled=True),
        preferred_element_type=jnp.float32,
    )
    return mixed.astype(jnp.bfloat16).reshape(1, -1, width)


def halves(array):
    high = array.astype(jnp.bfloat16)
    low = (array - high.astype(jnp.float32)).astype(jnp.bfloat16)
    return (high, low)


def product(left, right, dims=((1,), (0,))):
    def one(a, b):
        return lax.dot_general(a, b, (dims, ((), ())), preferred_element_type=jnp.float32)

    return one(left[0], right[0]) + (one(left[0], right[1]) + one(left[1], right[0]))


def mixer_kernel(
    size,
    span,
    group,
    proj_ref,
    pace_ref,
    base_ref,
    correction_ref,
    gain_ref,
    taps_ref,
    begin_ref,
    out_ref,
    local_ref,
    map_ref,
    carry_ref,
    add_ref,
    conv_ref,
):
    length = proj_ref.shape[0]
    heads = begin_ref.shape[0]
    wide = heads * size
    blocks = length // span
    kernel, channels = taps_ref.shape
    f32 = jnp.float32
    row = lax.broadcasted_iota(jnp.int32, (span, span), 0)
    col = lax.broadcasted_iota(jnp.int32, (span, span), 1)
    strict = (row > col).astype(f32)
    weak = (row >= col).astype(f32)
    masks = jnp.concatenate(
        [jnp.concatenate([strict, strict], axis=1), jnp.concatenate([weak, weak], axis=1)], axis=0
    )
    eye = (row == col).astype(f32)
    square = (
        lax.broadcasted_iota(jnp.int32, (size, size), 0)
        == lax.broadcasted_iota(jnp.int32, (size, size), 1)
    ).astype(f32)
    least = min(8, span)
    same = (row // least == col // least).astype(f32)
    merges = []
    width = least
    while width < span:
        merges.append(
            ((row // (2 * width) == col // (2 * width)) & (row // width != col // width)).astype(f32)
        )
        width = 2 * width
    weak_bf = weak.astype(jnp.bfloat16)

    def step(turn, _):
        items = []
        for part in range(group):
            block = turn * group + part
            rows = pl.ds(pl.multiple_of(block * span, span), span)
            query = proj_ref[rows, 0:wide].astype(f32)
            keys = proj_ref[rows, wide : 2 * wide].astype(f32)
            values = proj_ref[rows, 2 * wide : 3 * wide].astype(f32)
            decay_in = proj_ref[rows, 3 * wide : 4 * wide].astype(f32)
            log_keep = -jnp.exp(base_ref[...] + jnp.tanh(decay_in)) * pace_ref[rows, :]
            high = log_keep.astype(jnp.bfloat16)
            rest = log_keep - high.astype(f32)
            mid = rest.astype(jnp.bfloat16)
            low = (rest - mid.astype(f32)).astype(jnp.bfloat16)
            total = (
                jnp.dot(weak_bf, high, preferred_element_type=f32)
                + jnp.dot(weak_bf, mid, preferred_element_type=f32)
                + jnp.dot(weak_bf, low, preferred_element_type=f32)
            )
            last = total[span - 1 : span, :]
            lead = jnp.exp(total - log_keep)
            grown = jnp.exp(total)
            back = jnp.exp(-total)
            tail = jnp.exp(last - total)
            ended = jnp.exp(last)
            for head in range(heads):
                at = slice(head * size, (head + 1) * size)
                key = keys[:, at]
                unit = key * lax.rsqrt(
                    jnp.maximum(jnp.sum(key * key, axis=1, keepdims=True), 1.0)
                )
                write = unit * correction_ref[:, at]
                lead_remove = -unit * lead[:, at]
                lead_query = query[:, at] * grown[:, at]
                items.append(
                    dict(
                        at=(block, head),
                        value=values[:, at],
                        lead_remove=lead_remove,
                        lead_query=lead_query,
                        left=jnp.concatenate([lead_remove, lead_query], axis=0),
                        right=jnp.concatenate([write * back[:, at], key * back[:, at]], axis=0),
                        tail_write=write * tail[:, at],
                        tail_key=key * tail[:, at],
                        ended=ended[:, at],
                    )
                )
        for item in items:
            item["pair"] = (
                product(halves(item["left"]), halves(item["right"]), ((1,), (1,))) * masks
            )
        for item in items:
            item["system"] = item["pair"][:span, :span]
            item["power"] = halves(item["system"] * same)
            item["inverse"] = eye + item["system"] * same
        width = 2
        while width < least:
            for item in items:
                item["power"] = halves(product(item["power"], item["power"]))
            for item in items:
                item["inverse"] = item["inverse"] + product(
                    halves(item["inverse"]), item["power"]
                )
            width = 2 * width
        for item in items:
            padded = jnp.concatenate([jnp.zeros_like(item["value"]), item["value"]], axis=0)
            item["mixed"] = product(halves(item["pair"]), halves(padded))
        for merge in merges:
            for item in items:
                item["inside"] = halves(item["inverse"])
                item["next"] = halves(product(halves(item["system"] * merge), item["inside"]))
            for item in items:
                item["inverse"] = item["inverse"] + product(item["inside"], item["next"])
        for item in items:
            right_side = jnp.concatenate([item["mixed"][:span], item["lead_remove"]], axis=1)
            item["solved"] = halves(product(halves(item["inverse"]), halves(right_side)))
        for item in items:
            block, head = item["at"]
            seen = product(halves(item["pair"][span:, :span]), item["solved"])
            local_ref[head, block] = seen[:, :size] + item["mixed"][span:]
            map_ref[head, block] = item["lead_query"] + seen[:, size:]
            carried = product(item["solved"], halves(item["tail_write"]), ((0,), (0,)))
            carry_ref[head, block] = carried[size:] + square * item["ended"]
            add_ref[head, block] = carried[:size] + product(
                halves(item["value"]), halves(item["tail_key"]), ((0,), (0,))
            )
        return 0

    lax.fori_loop(0, blocks // group, step, 0)

    states = [begin_ref[head] for head in range(heads)]
    for block in range(blocks):
        rows = pl.ds(block * span, span)
        gate = proj_ref[rows, 4 * wide : 5 * wide].astype(f32)
        pieces = []
        for head in range(heads):
            at = slice(head * size, (head + 1) * size)
            state = halves(states[head])
            out = local_ref[head, block] + product(
                halves(map_ref[head, block]), state, ((1,), (1,))
            )
            states[head] = product(state, halves(carry_ref[head, block])) + add_ref[head, block]
            centered = out - jnp.mean(out, axis=1, keepdims=True)
            variance = jnp.mean(centered * centered, axis=1, keepdims=True)
            pieces.append(centered * lax.rsqrt(variance + GROUP_FLOOR))
        grouped = jnp.concatenate(pieces, axis=1) * gain_ref[...]
        out_ref[rows, 0:wide] = (grouped * gate * jax.nn.sigmoid(gate)).astype(out_ref.dtype)

    lead_rows = conv_ref.shape[0] - length
    conv_ref[0:lead_rows, :] = jnp.zeros((lead_rows, channels), f32)
    conv_at = 5 * wide
    for block in range(blocks):
        rows = pl.ds(block * span, span)
        value = proj_ref[rows, conv_at : conv_at + channels].astype(f32)
        admit = proj_ref[rows, conv_at + channels : conv_at + 2 * channels].astype(f32)
        conv_ref[pl.ds(lead_rows + block * span, span), :] = (
            (value * jax.nn.sigmoid(admit)).astype(jnp.bfloat16).astype(f32)
        )
    for block in range(blocks):
        total = jnp.zeros((span, channels), f32)
        for place in range(kernel):
            first = lead_rows - (kernel - 1) + block * span + place
            total = total + taps_ref[place : place + 1, :] * conv_ref[pl.ds(first, span), :]
        rows = pl.ds(block * span, span)
        out_ref[rows, wide : wide + channels] = total.astype(out_ref.dtype)
        out_ref[rows, wide + channels : wide + 2 * channels] = proj_ref[
            rows, conv_at + 2 * channels : conv_at + 3 * channels
        ]


def mixer(projected, pace, base, correction, gain, taps, begin):
    length = projected.shape[0]
    heads, size, _ = begin.shape
    kernel, channels = taps.shape
    span = 64
    blocks = length // span
    group = next(n for n in (4, 3, 2, 1) if blocks % n == 0)
    lead_rows = -(-(kernel - 1) // 8) * 8
    maps = pltpu.VMEM((heads, blocks, size, size), jnp.float32)
    return pl.pallas_call(
        functools.partial(mixer_kernel, size, span, group),
        out_shape=jax.ShapeDtypeStruct((length, heads * size + 2 * channels), jnp.bfloat16),
        in_specs=[pl.BlockSpec(memory_space=pltpu.VMEM)] * 7,
        out_specs=pl.BlockSpec(memory_space=pltpu.VMEM),
        scratch_shapes=[
            pltpu.VMEM((heads, blocks, span, size), jnp.float32),
            pltpu.VMEM((heads, blocks, span, size), jnp.float32),
            maps,
            maps,
            pltpu.VMEM((lead_rows + length, channels), jnp.float32),
        ],
        compiler_params=pltpu.CompilerParams(vmem_limit_bytes=48 * 1024 * 1024),
        cost_estimate=pl.CostEstimate(
            flops=60_000_000_000, bytes_accessed=4_000_000, transcendentals=0
        ),
        name="mixer",
    )(projected, pace, base, correction, gain, taps, begin)


def collect_kernel(
    along,
    normed_ref,
    parted_ref,
    pace_ref,
    rows_ref,
    proj_ref,
    paces_ref,
    joined_ref,
    sequence,
    weights,
    w_send,
    w_recv,
    t_send,
    t_recv,
    p_send,
    p_recv,
    y_send,
    y_recv,
    c_send,
    c_recv,
    r_send,
    r_recv,
    x_send,
    x_recv,
    o_send,
    o_recv,
):
    place = lax.axis_index("sp")
    seat = lax.axis_index("fs")
    side = lax.axis_index("tp")
    depth = parted_ref.shape[1]
    length = normed_ref.shape[0]
    half = length // 2
    near = seat + 1 - 2 * lax.rem(seat, 2)
    far = lax.rem(seat + 2, 4)
    other = 1 - side

    def ahead(steps):
        return lax.rem(place + steps, along)

    def behind(steps):
        return lax.rem(place + along - steps, along)

    def block(sp_at, fs_at):
        return weights.at[pl.ds(pl.multiple_of((sp_at * 4 + fs_at) * depth, depth), depth)]

    def tokens_at(sp_at, side_at):
        return sequence.at[
            pl.ds(pl.multiple_of(sp_at * length + side_at * half, half), half)
        ]

    def send(source, target, send_sem, recv_sem, where):
        copy = pltpu.make_async_remote_copy(
            src_ref=source,
            dst_ref=target,
            send_sem=send_sem,
            recv_sem=recv_sem,
            device_id=where,
            device_id_type=pl.DeviceIdType.MESH,
        )
        copy.start()
        sent.append(copy)

    def arrive(target, send_sem, recv_sem, where):
        pltpu.make_async_remote_copy(
            src_ref=target,
            dst_ref=target,
            send_sem=send_sem,
            recv_sem=recv_sem,
            device_id=where,
            device_id_type=pl.DeviceIdType.MESH,
        ).wait_recv()

    sent = []
    barrier = pltpu.get_barrier_semaphore()
    partners = [{"sp": ahead(s)} for s in range(1, along)]
    partners += [{"fs": near}, {"fs": far}, {"tp": other}]
    for partner in partners:
        pl.semaphore_signal(
            barrier, inc=1, device_id=partner, device_id_type=pl.DeviceIdType.MESH
        )
    pl.semaphore_wait(barrier, len(partners))

    order = sorted(range(1, along), key=lambda s: min(s, along - s))
    own = parted_ref.at[place]
    for s in order:
        send(
            parted_ref.at[ahead(s)], block(place, seat), w_send.at[s], w_recv.at[s], {"sp": ahead(s)}
        )
    send(own, block(place, seat), y_send.at[0], y_recv.at[0], {"fs": far})
    send(own, block(place, seat), c_send.at[0], c_recv.at[0], {"fs": near})
    for s in order:
        send(pace_ref, paces_ref.at[place], p_send.at[s], p_recv.at[s], {"sp": ahead(s)})
    for s in order:
        send(
            normed_ref.at[pl.ds(pl.multiple_of(side * half, half), half)],
            tokens_at(place, side),
            t_send.at[s],
            t_recv.at[s],
            {"sp": ahead(s)},
        )
    send(rows_ref, joined_ref.at[side], o_send.at[0], o_recv.at[0], {"tp": other})

    block(place, seat)[...] = parted_ref[place]
    sequence[pl.ds(pl.multiple_of(place * length, length), length), :] = normed_ref[...]
    joined_ref[side] = rows_ref[...]
    paces_ref[place] = pace_ref[...]

    def weights_on(s):
        here = block(behind(s), seat)
        arrive(here, w_send.at[s], w_recv.at[s], {"sp": ahead(s)})
        send(here, here, y_send.at[s], y_recv.at[s], {"fs": far})
        send(here, here, c_send.at[s], c_recv.at[s], {"fs": near})

    def relay(s):
        here = block(behind(s), far)
        arrive(here, y_send.at[s], y_recv.at[s], {"fs": far})
        send(here, here, r_send.at[s], r_recv.at[s], {"fs": near})

    def tokens_on(s):
        here = tokens_at(behind(s), side)
        arrive(here, t_send.at[s], t_recv.at[s], {"sp": ahead(s)})
        send(here, here, x_send.at[s], x_recv.at[s], {"tp": other})

    for s in order[:2]:
        weights_on(s)
    relay(0)
    for s in order[2:]:
        weights_on(s)
    for at, s in enumerate(order):
        relay(s)
        tokens_on(s)

    for s in [0] + order:
        arrive(block(behind(s), near), c_send.at[s], c_recv.at[s], {"fs": near})
        beyond = lax.rem(near + 2, 4)
        arrive(block(behind(s), beyond), r_send.at[s], r_recv.at[s], {"fs": near})
    for s in order:
        arrive(tokens_at(behind(s), other), x_send.at[s], x_recv.at[s], {"tp": other})
        arrive(paces_ref.at[behind(s)], p_send.at[s], p_recv.at[s], {"sp": ahead(s)})
    arrive(joined_ref.at[other], o_send.at[0], o_recv.at[0], {"tp": other})
    for copy in sent:
        copy.wait_send()

    total = sequence.shape[0]
    tile = next(n for n in (256, 192, 128, 96, 64, 32, 16) if total % n == 0)

    def multiply(turn, _):
        at = pl.ds(pl.multiple_of(turn * tile, tile), tile)
        proj_ref[at, :] = jnp.dot(
            sequence[at, :], weights[...], preferred_element_type=jnp.float32
        ).astype(proj_ref.dtype)
        return 0

    lax.fori_loop(0, total // tile, multiply, 0)


def collect(normed, parted, pace, rows):
    along = parted.shape[0]
    length, width = normed.shape
    columns = parted.shape[2]
    pair = pltpu.SemaphoreType.DMA((along,))
    single = pltpu.SemaphoreType.DMA((1,))
    return pl.pallas_call(
        functools.partial(collect_kernel, along),
        out_shape=(
            jax.ShapeDtypeStruct((along * length, columns), jnp.bfloat16),
            jax.ShapeDtypeStruct((along,) + pace.shape, pace.dtype),
            jax.ShapeDtypeStruct((2,) + rows.shape, rows.dtype),
        ),
        in_specs=[pl.BlockSpec(memory_space=pltpu.VMEM)] * 4,
        out_specs=(pl.BlockSpec(memory_space=pltpu.VMEM),) * 3,
        scratch_shapes=[
            pltpu.VMEM((along * length, width), jnp.bfloat16),
            pltpu.VMEM((width, columns), jnp.bfloat16),
        ]
        + [pair] * 14
        + [single] * 2,
        compiler_params=pltpu.CompilerParams(
            collective_id=0, has_side_effects=True, vmem_limit_bytes=48 * 1024 * 1024
        ),
        cost_estimate=pl.CostEstimate(
            flops=60_000_000_000, bytes_accessed=8_000_000, transcendentals=0
        ),
        name="collect",
    )(normed, parted, pace, rows)


def own_part(array, axis, count, dim):
    part = array.shape[dim] // count
    return lax.dynamic_slice_in_dim(array, lax.axis_index(axis) * part, part, dim)


def whole_sequence_body(
    tokens,
    decay_pace,
    start_state,
    norm_gain,
    conv_value,
    conv_admit,
    conv_gate,
    state_query,
    state_key,
    state_value,
    state_decay,
    state_gate,
    conv_taps,
    conv_gain,
    point_weight,
    decay_base,
    correction,
    group_gain,
    output_conv,
    output_state,
):
    along = lax.axis_size("sp")
    groups = lax.axis_size("tp")
    width = tokens.shape[-1]
    rows = tokens.reshape(-1, width)
    depth = conv_value.shape[0]

    shards = (
        state_query,
        state_key,
        state_value,
        state_decay,
        state_gate,
        conv_value,
        conv_admit,
        conv_gate,
    )
    parted = jnp.concatenate(
        [shard.reshape(depth, along, -1).transpose(1, 0, 2) for shard in shards], axis=2
    )
    floats = rows.astype(jnp.float32)
    inverse = lax.rsqrt(jnp.mean(floats * floats, axis=1, keepdims=True) + NORM_FLOOR)
    normed = (floats * inverse * norm_gain).astype(jnp.bfloat16)
    output_weights = lax.all_gather(
        jnp.concatenate([output_conv, output_state], axis=0), ("sp", "fs"), axis=1, tiled=True
    )
    columns = output_conv.shape[1]
    gain_rows = conv_gain.astype(jnp.bfloat16).reshape(-1, columns)
    spare = -gain_rows.shape[0] % 16
    sent_rows = jnp.concatenate(
        [gain_rows, jnp.zeros((spare, columns), jnp.bfloat16)], axis=0
    )
    span = rows.shape[0]
    lanes = -(-span // 128) * 128
    sent_pace = jnp.broadcast_to(
        jnp.pad(decay_pace.reshape(1, -1), ((0, 0), (0, lanes - span))), (8, lanes)
    )
    projected, paces, joined = collect(normed, parted, sent_pace, sent_rows)
    pace = paces[:, 0, :span].reshape(-1, 1)

    channels = conv_value.shape[1]
    mixed_in = mixer(
        projected,
        pace,
        own_part(decay_base[None], "sp", along, 1),
        own_part(correction[None], "sp", along, 1),
        own_part(group_gain[None], "sp", along, 1),
        own_part(conv_taps, "sp", along, 1),
        own_part(start_state[0], "sp", along, 0),
    )
    owners = along * groups
    heads_wide = state_query.shape[1] // along
    part = channels // along
    sent = mixed_in.reshape(owners, -1, mixed_in.shape[1])
    moved = lax.all_to_all(sent, ("sp", "tp"), split_axis=0, concat_axis=0, tiled=True)
    own_rows = moved.shape[1]
    moved = moved.reshape(along, groups, own_rows, -1).transpose(2, 1, 0, 3)
    state_out = moved[..., :heads_wide].reshape(own_rows, groups, -1)
    conv_sum = (
        moved[..., heads_wide : heads_wide + part].reshape(own_rows, -1).astype(jnp.float32)
    )
    gate_conv = moved[..., heads_wide + part :].reshape(own_rows, -1).astype(jnp.float32)

    whole_gain = joined[:, : gain_rows.shape[0]].reshape(-1).astype(jnp.float32)

    mean = jnp.mean(conv_sum, axis=1, keepdims=True)
    spread = jnp.mean(conv_sum * conv_sum, axis=1, keepdims=True) - mean * mean
    shaped = jax.nn.silu(
        (conv_sum - mean) * lax.rsqrt(spread + CHANNEL_FLOOR) * whole_gain
    ).astype(jnp.bfloat16)
    pointwise = jnp.dot(shaped, point_weight, preferred_element_type=jnp.float32)
    conv_out = (pointwise * jax.nn.silu(gate_conv)).astype(jnp.bfloat16)
    joined_rows = jnp.concatenate(
        [
            conv_out.reshape(own_rows, groups, -1).transpose(1, 0, 2),
            state_out.reshape(own_rows, groups, -1).transpose(1, 0, 2),
        ],
        axis=2,
    )
    traded = lax.all_to_all(joined_rows, "tp", split_axis=0, concat_axis=0, tiled=True)
    partial = jnp.dot(
        traded.reshape(groups * own_rows, -1), output_weights, preferred_element_type=jnp.float32
    ).astype(jnp.bfloat16)
    parts = lax.all_to_all(
        partial.reshape(groups, own_rows, width), "tp", split_axis=0, concat_axis=0, tiled=True
    )
    mixed = jnp.sum(parts.astype(jnp.float32), axis=0)
    return mixed.astype(jnp.bfloat16).reshape(1, -1, width)


def dispatch(*arrays):
    along = lax.axis_size("sp")
    tokens, start_state, conv_value, conv_gain, output_conv = (
        arrays[0],
        arrays[2],
        arrays[4],
        arrays[13],
        arrays[18],
    )
    fits = (
        along > 2
        and lax.axis_size("fs") == 4
        and lax.axis_size("tp") == 2
        and tokens.shape[1] % 32 == 0
        and start_state.shape[1] % along == 0
        and (conv_value.shape[1] // along) % 64 == 0
        and conv_gain.shape[0] % output_conv.shape[1] == 0
        and (tokens.shape[1] * along) % 64 == 0
    )
    return (whole_sequence_body if fits else body)(*arrays)


def solution(mesh):
    return jax.shard_map(
        dispatch,
        mesh=mesh,
        in_specs=(
            P("fs", "sp", None),
            P("fs", "sp"),
            P("fs", "tp", None, None),
            P(),
            P(("sp", "fs"), "tp"),
            P(("sp", "fs"), "tp"),
            P(("sp", "fs"), "tp"),
            P(("sp", "fs"), "tp"),
            P(("sp", "fs"), "tp"),
            P(("sp", "fs"), "tp"),
            P(("sp", "fs"), "tp"),
            P(("sp", "fs"), "tp"),
            P(None, "tp"),
            P("tp"),
            P(),
            P("tp"),
            P("tp"),
            P("tp"),
            P("tp", ("sp", "fs")),
            P("tp", ("sp", "fs")),
        ),
        out_specs=P("fs", ("sp", "tp"), None),
        check_vma=False,
    )
```
